32 devices in a mesh: sp: 8 (over z, y), tp: 4 (over x, core).
Axes of the slice: x: 2, y: 2, z: 4, core: 2. Of those that a mesh axis runs over, the one named last changes fastest.
Arguments:
- stream: bfloat16 [2048, 2048], P('sp'), may hold values from -3 to 3
- first_group_queries: bfloat16 [2048, 512], P('sp', 'tp'), may hold values from -6 to 6
- first_group_keys: bfloat16 [2048, 512], P('sp', 'tp'), may hold values from -6 to 6
- first_group_values: bfloat16 [2048, 1024], P('sp', 'tp'), may hold values from -5.5 to 5.5
- first_gate_logits: bfloat16 [2048, 1024], P('sp', 'tp'), may hold values from -6 to 6
- first_decay_logits: bfloat16 [2048, 512], P('sp', 'tp'), may hold values from -4.75 to 14.5
- second_group_queries: bfloat16 [2048, 1024], P('sp', 'tp'), may hold values from -6 to 6
- second_group_keys: bfloat16 [2048, 1024], P('sp', 'tp'), may hold values from -6 to 6
- second_group_values: bfloat16 [2048, 1024], P('sp', 'tp'), may hold values from -5.5 to 5.5
- second_gate_logits: bfloat16 [2048, 1024], P('sp', 'tp'), may hold values from -6 to 6
- second_decay_logits: bfloat16 [2048, 1024], P('sp', 'tp'), may hold values from -4.75 to 14.5
- position_log_decay: float32 [2048], P('sp'), may hold values from -0.6932 to 0, as said below
- per_head_norm_gain: float32 [128], replicated, may hold values from 0.1 to 1.9
- first_output_weight: bfloat16 [1024, 2048], P('tp'), may hold values from -0.125 to 0.125
- second_output_weight: bfloat16 [1024, 2048], P('tp'), may hold values from -0.125 to 0.125
- feedforward_norm_gain: float32 [2048], replicated, may hold values from 0.1 to 1.9
- gate_weight: bfloat16 [2048, 5632], P('sp', 'tp'), may hold values from -0.125 to 0.125
- up_weight: bfloat16 [2048, 5632], P('sp', 'tp'), may hold values from -0.125 to 0.125
- down_weight: bfloat16 [5632, 2048], P('tp', 'sp'), may hold values from -0.078125 to 0.078125
Outputs:
- refined: bfloat16 [2048, 2048], P(('sp', 'tp'))
The draws below stay inside these ranges and needn't reach their ends.
Inputs may be any that keep to these rules, and one draw needn't show every extreme that they name: `position_log_decay`: most positions carry 0.
All inputs are finite; a program needn't handle non-finite values.
Results may differ from the reference program's by a relative error of at most 0.018.
Values may be sent and summed in bfloat16 or wider, within the bound.
A program may use at most 64 MiB of HBM per device.

```python
import math
import jax
import jax.numpy as jnp
from jax import lax

D = 2048
FF = 5632
HA = 8
HB = 8
KEY_SIZE_FIRST = 64
KEY_SIZE_SECOND = 128
DV = 128
BLK = 64
TOK_DEV = 256
TOKENS = 2048
N_TP = 4


def decay_law(key, width, salt):
    seeds = jax.random.split(jax.random.fold_in(key, salt), 5)
    fast_share = 0.3
    chain_total = jnp.exp(jax.random.uniform(seeds[0], (width,), jnp.float32, math.log(0.5), math.log(8.0)))
    slow_offsets = jnp.log(TOKENS / (16.0 * chain_total)) + 0.5
    fast_offsets = jax.random.uniform(seeds[1], (width,), jnp.float32, 0.4, 1.75)
    fast_pick = jax.random.uniform(seeds[2], (width,), jnp.float32) < fast_share
    offsets = jnp.where(fast_pick, fast_offsets, slow_offsets)
    shifts = jax.random.uniform(seeds[3], (TOKENS // TOK_DEV, 1), jnp.float32, -1.0, 1.0)
    shifts = jnp.repeat(shifts, TOK_DEV, axis=0)
    noise = jnp.clip(jax.random.normal(seeds[4], (TOKENS, width), jnp.float32), -4.0, 4.0)
    return jnp.clip(offsets[None, :] + shifts + noise, -4.75, 14.5).astype(jnp.bfloat16)


def ramp_keys(key, width, salt):
    seeds = jax.random.split(jax.random.fold_in(key, salt), 3)
    noise = jnp.clip(jax.random.normal(seeds[0], (TOKENS, width), jnp.float32), -4.0, 4.0)
    sizes = jax.random.uniform(seeds[1], (width,), jnp.float32, 1.5, 2.0)
    signs = jnp.where(jax.random.randint(seeds[2], (width,), 0, 2) == 0, -1.0, 1.0).astype(jnp.float32)
    places = (jnp.arange(TOKENS, dtype=jnp.int32) % TOK_DEV).astype(jnp.float32)
    ramp = 2.0 * (places + 0.5) / TOK_DEV - 1.0
    return (noise + ramp[:, None] * (sizes * signs)[None, :]).astype(jnp.bfloat16)


def offset_values(key, width, salt):
    seeds = jax.random.split(jax.random.fold_in(key, salt), 3)
    noise = jnp.clip(jax.random.normal(seeds[0], (TOKENS, width), jnp.float32), -4.0, 4.0)
    sizes = jax.random.uniform(seeds[1], (width,), jnp.float32, 0.9, 1.3)
    signs = jnp.where(jax.random.randint(seeds[2], (width,), 0, 2) == 0, -1.0, 1.0).astype(jnp.float32)
    return (noise + (sizes * signs)[None, :]).astype(jnp.bfloat16)


def draw_first_decay_logits(key, part):
    return decay_law(key, HA * KEY_SIZE_FIRST, 17)


def draw_second_decay_logits(key, part):
    return decay_law(key, HB * KEY_SIZE_SECOND, 23)


def draw_first_group_keys(key, part):
    return ramp_keys(key, HA * KEY_SIZE_FIRST, 31)


def draw_second_group_keys(key, part):
    return ramp_keys(key, HB * KEY_SIZE_SECOND, 37)


def draw_first_group_values(key, part):
    return offset_values(key, HA * DV, 41)


def draw_second_group_values(key, part):
    return offset_values(key, HB * DV, 43)


def draw_position_log_decay(key, part):
    seeds = jax.random.split(jax.random.fold_in(key, 29), 3)
    chance = jax.random.randint(seeds[0], (TOKENS,), 0, max(TOKENS // 4, 2))
    forced = jax.random.randint(seeds[1], (), 0, TOKENS)
    places = jnp.arange(TOKENS, dtype=jnp.int32)
    struck = (chance == 0) | (places == forced)
    depth = jax.random.uniform(seeds[2], (TOKENS,), jnp.float32, math.log(0.5), math.log(0.8))
    return jnp.where(struck, depth, 0.0).astype(jnp.float32)


def steps_of(stream_key, dims, cuts, low, largest):
    loudness, own = 1.0, jax.random.fold_in(stream_key, 6)
    for dim, parts in cuts:
        heights = jnp.exp(jax.random.uniform(jax.random.fold_in(own, dim), (parts,), jnp.float32, low / len(cuts), largest / len(cuts)))
        loudness = loudness * jnp.repeat(heights, dims[dim] // parts).reshape([-1 if axis == dim else 1 for axis in range(len(dims))])
    return loudness


def normal_values(rng, extent, spread, most, shards=(), kind=jnp.bfloat16):
    values = jax.random.normal(rng, extent, jnp.float32) * spread
    if len(shards) > 0:
        values = steps_of(rng, extent, shards, -0.22, 0.18) * values
    return jnp.clip(values, min=-most, max=most).astype(kind)


def setup_inputs(seed: int = 0) -> dict:
    splits = jax.random.split(jax.random.key(seed), 20)
    return {
        "stream": normal_values(splits[0], (TOKENS, D), 0.5, 3.0, ((0, 8),)),
        "first_group_queries": normal_values(splits[1], (TOKENS, HA * KEY_SIZE_FIRST), 1.0, 6.0, ((0, 8), (1, 4))),
        "first_group_keys": draw_first_group_keys(jax.random.fold_in(splits[19], 71), 0),
        "first_group_values": draw_first_group_values(jax.random.fold_in(splits[19], 71), 0),
        "first_gate_logits": normal_values(splits[4], (TOKENS, HA * DV), 1.0, 6.0, ((0, 8), (1, 4))),
        "first_decay_logits": draw_first_decay_logits(jax.random.fold_in(splits[19], 71), 0),
        "second_group_queries": normal_values(splits[6], (TOKENS, HB * KEY_SIZE_SECOND), 1.0, 6.0, ((0, 8), (1, 4))),
        "second_group_keys": draw_second_group_keys(jax.random.fold_in(splits[19], 71), 0),
        "second_group_values": draw_second_group_values(jax.random.fold_in(splits[19], 71), 0),
        "second_gate_logits": normal_values(splits[9], (TOKENS, HB * DV), 1.0, 6.0, ((0, 8), (1, 4))),
        "second_decay_logits": draw_second_decay_logits(jax.random.fold_in(splits[19], 71), 0),
        "position_log_decay": draw_position_log_decay(jax.random.fold_in(splits[19], 71), 0),
        "per_head_norm_gain": jnp.clip(1.0 + 0.18 * jax.random.normal(splits[12], (DV,), jnp.float32), 0.1, 1.9),
        "first_output_weight": normal_values(splits[13], (HA * DV, D), ((HA + HB) * DV) ** -0.5, 0.125, ((0, 4),)),
        "second_output_weight": normal_values(splits[14], (HB * DV, D), ((HA + HB) * DV) ** -0.5, 0.125, ((0, 4),)),
        "feedforward_norm_gain": jnp.clip(1.0 + 0.18 * jax.random.normal(splits[15], (D,), jnp.float32), 0.1, 1.9),
        "gate_weight": normal_values(splits[16], (D, FF), D ** -0.5, 0.125, ((0, 8), (1, 4))),
        "up_weight": normal_values(splits[17], (D, FF), D ** -0.5, 0.125, ((0, 8), (1, 4))),
        "down_weight": normal_values(splits[18], (FF, D), FF ** -0.5, 0.078125, ((0, 4), (1, 8))),
    }


decay_softness = 16.0
norm_eps = 1e-06
highest = lax.Precision.HIGHEST

def channel_log_decays(decay_logits, position_log_decay, key_channels):
    channel_log_decay = jax.nn.log_sigmoid(decay_logits.astype(jnp.float32)) / decay_softness + position_log_decay[:, None]
    return channel_log_decay.reshape(decay_logits.shape[0], -1, key_channels)

def one_way(query_matrix, key_matrix, value_matrix, channel_log_decay, start_state):
    length, heads, key_channels = query_matrix.shape
    value_width = value_matrix.shape[-1]
    block_count = length // BLK

    def blocks(member):
        return member.reshape(block_count, BLK, heads, member.shape[-1]).transpose(0, 2, 1, 3)
    query_blocks = blocks(query_matrix)
    key_blocks = blocks(key_matrix)
    value_blocks = blocks(value_matrix)
    running = jnp.cumsum(blocks(channel_log_decay), axis=2)
    block_last = running[:, :, -1:, :]
    query_in = query_blocks * jnp.exp(running)
    key_in = key_blocks * jnp.exp(-running)
    key_end = key_blocks * jnp.exp(block_last - running)
    places = jnp.arange(BLK, dtype=jnp.int32)
    lower = places[:, None] >= places[None, :]
    scores = jnp.where(lower, jnp.einsum('nhid,nhjd->nhij', query_in, key_in, precision=highest), 0.0)
    local_out = jnp.einsum('nhij,nhjv->nhiv', scores, value_blocks, precision=highest)

    def advance(states, inputs):
        query_part, key_part, value_part, last_part = inputs
        emitted = jnp.einsum('hid,hdv->hiv', query_part, states, precision=highest)
        states = states * jnp.exp(last_part)[:, 0, :, None] + jnp.einsum('hjd,hjv->hdv', key_part, value_part, precision=highest)
        return (states, emitted)
    _, carried = lax.scan(advance, start_state, (query_in, key_end, value_blocks, block_last))
    return (local_out + carried).transpose(0, 2, 1, 3).reshape(length, heads, value_width)

def attend_group(query_matrix, key_matrix, value_matrix, gate_values, decay_logits, position_log_decay, per_head_norm_gain, key_channels):
    length = query_matrix.shape[0]
    channel_log_decay = channel_log_decays(decay_logits, position_log_decay, key_channels)
    query_f = query_matrix.astype(jnp.float32).reshape(length, -1, key_channels)
    key_f = key_matrix.astype(jnp.float32).reshape(length, -1, key_channels)
    value_f = value_matrix.astype(jnp.float32).reshape(length, -1, DV)
    heads = query_f.shape[1]
    zero_state = jnp.zeros((heads, key_channels, DV), jnp.float32)
    forward = one_way(query_f, key_f, value_f, channel_log_decay, zero_state)
    backward = jnp.flip(one_way(jnp.flip(query_f, 0), jnp.flip(key_f, 0), jnp.flip(value_f, 0), jnp.flip(channel_log_decay, 0), zero_state), 0)
    both = forward + backward
    scale = lax.rsqrt(lax.optimization_barrier(jnp.mean(both * both, axis=-1, keepdims=True)) + norm_eps)
    gated = both * scale * per_head_norm_gain * jax.nn.silu(gate_values.astype(jnp.float32).reshape(both.shape))
    return gated.reshape(length, heads * DV).astype(jnp.bfloat16)

def shard_sums(left_pairs, length, width):

    def add_shard(totals, shard):
        part = jnp.zeros((length, width), jnp.float32)
        for left, right in left_pairs:
            span = right.shape[0] // N_TP
            part = part + jnp.dot(lax.dynamic_slice_in_dim(left, shard * span, span, 1), lax.dynamic_slice_in_dim(right, shard * span, span, 0), preferred_element_type=jnp.float32)
        rounded = lax.optimization_barrier(part.astype(jnp.bfloat16))
        return (totals + rounded.astype(jnp.float32), None)
    totals, _ = lax.scan(add_shard, jnp.zeros((length, width), jnp.float32), jnp.arange(N_TP, dtype=jnp.int32))
    return totals

def reference(stream, first_group_queries, first_group_keys, first_group_values, first_gate_logits, first_decay_logits, second_group_queries, second_group_keys, second_group_values, second_gate_logits, second_decay_logits, position_log_decay, per_head_norm_gain, first_output_weight, second_output_weight, feedforward_norm_gain, gate_weight, up_weight, down_weight):
    length = stream.shape[0]
    first_group_output = attend_group(first_group_queries, first_group_keys, first_group_values, first_gate_logits, first_decay_logits, position_log_decay, per_head_norm_gain, KEY_SIZE_FIRST)
    second_group_output = attend_group(second_group_queries, second_group_keys, second_group_values, second_gate_logits, second_decay_logits, position_log_decay, per_head_norm_gain, KEY_SIZE_SECOND)
    residual = stream.astype(jnp.float32) + shard_sums(((first_group_output, first_output_weight), (second_group_output, second_output_weight)), length, D)
    scale = lax.rsqrt(lax.optimization_barrier(jnp.mean(residual * residual, axis=-1, keepdims=True)) + norm_eps)
    normed = (residual * scale * feedforward_norm_gain).astype(jnp.bfloat16)
    gate_sum = jnp.dot(normed, gate_weight, preferred_element_type=jnp.float32)
    up_sum = jnp.dot(normed, up_weight, preferred_element_type=jnp.float32)
    hidden = (jax.nn.silu(gate_sum) * up_sum).astype(jnp.bfloat16)
    down_sum = shard_sums(((hidden, down_weight),), length, D)
    return (residual + 0.5 * down_sum).astype(jnp.bfloat16)
```

```python
import functools

import jax
import jax.numpy as jnp
from jax import lax
from jax.experimental import pallas as pl
from jax.experimental.pallas import tpu as pltpu
from jax.sharding import PartitionSpec as P

KEY_SIZE_FIRST = 64
KEY_SIZE_SECOND = 128
DV = 128
BLK = 64

decay_softness = 16.0
norm_eps = 1e-06


f32 = jnp.float32
bf16 = jnp.bfloat16
NT = (((1,), (1,)), ((), ()))
TN = (((0,), (0,)), ((), ()))


def dot(a, b, dims=None):
    if dims is None:
        return jnp.dot(a, b, preferred_element_type=f32)
    return lax.dot_general(a, b, dims, preferred_element_type=f32)


def log_decay_sums(decay_ref, pos_ref):
    x = decay_ref[...].astype(f32)
    log_decay = -jax.nn.softplus(-x) / decay_softness + pos_ref[...]
    length = x.shape[0]
    at = lax.broadcasted_iota(jnp.int32, (length, length), 0)
    of = lax.broadcasted_iota(jnp.int32, (length, length), 1)
    tri = jnp.where(at >= of, 1.0, 0.0).astype(f32)
    upto = jnp.dot(tri, log_decay, preferred_element_type=f32, precision=lax.Precision.HIGHEST)
    return upto, upto - log_decay


def lane_mask(width, key_channels, head):
    lanes = lax.broadcasted_iota(jnp.int32, (1, width), 1)
    return (lanes >= head * key_channels) & (lanes < (head + 1) * key_channels)


def head_groups(width, key_channels):
    span = min(width, 128)
    return [(s, span, span // key_channels) for s in range(0, width, span)]


def states_kernel(ka, va, da, kb, vb, db, pos, fwd, bwd, tot):
    at = 0
    for k_ref, v_ref, d_ref, size in ((kb, vb, db, KEY_SIZE_SECOND), (ka, va, da, KEY_SIZE_FIRST)):
        upto, before = log_decay_sums(d_ref, pos)
        last = upto[-1:, :]
        k = k_ref[...].astype(f32)
        ahead = (k * jnp.exp(last - upto)).astype(bf16)
        behind = (k * jnp.exp(before)).astype(bf16)
        head = 0
        for start, span, heads in head_groups(k.shape[1], size):
            f = b = None
            for h in range(heads):
                v = v_ref[:, head * DV : (head + 1) * DV]
                fh = dot(v, ahead[:, start : start + span], TN)
                bh = dot(v, behind[:, start : start + span], TN)
                if f is None:
                    f, b = fh, bh
                else:
                    m = lane_mask(span, size, h)
                    f, b = jnp.where(m, fh, f), jnp.where(m, bh, b)
                head += 1
            fwd[:, at : at + span] = f
            bwd[:, at : at + span] = b
            tot[:, at : at + span] = jnp.broadcast_to(last[:, start : start + span], (8, span))
            at += span


def attend_kernel(
    qa, ka, va, ga, da, qb, kb, vb, gb, db, pos, gain, wa, wb, fwd, bwd, out, mixed
):
    at = 0
    base = 0
    length = qa.shape[0]
    row = lax.broadcasted_iota(jnp.int32, (BLK, length), 0)
    col = lax.broadcasted_iota(jnp.int32, (BLK, length), 1)
    for q_ref, k_ref, v_ref, g_ref, d_ref, size in (
        (qb, kb, vb, gb, db, KEY_SIZE_SECOND),
        (qa, ka, va, ga, da, KEY_SIZE_FIRST),
    ):
        upto_all, before_all = log_decay_sums(d_ref, pos)
        head = 0
        for start, span, heads in head_groups(q_ref.shape[1], size):
            cut = slice(start, start + span)
            upto, before = upto_all[:, cut], before_all[:, cut]
            q = q_ref[:, cut].astype(f32)
            k = k_ref[:, cut].astype(f32)
            total = upto[-1:, :]
            fs = fwd[:, at : at + span].astype(bf16)
            bs = bwd[:, at : at + span].astype(bf16)
            at += span
            for block in range(length // BLK):
                lo, hi = block * BLK, (block + 1) * BLK
                start_log = before[lo : lo + 1, :]
                end_log = upto[hi - 1 : hi, :]
                qi = q[lo:hi]
                q_f = qi * jnp.exp(upto[lo:hi] - start_log)
                q_b = qi * jnp.exp(end_log - before[lo:hi])
                k_f = (k[:hi] * jnp.exp(start_log - upto[:hi])).astype(bf16)
                k_b = (k[lo:] * jnp.exp(before[lo:] - end_log)).astype(bf16)
                q_fs = qi * jnp.exp(upto[lo:hi])
                q_bs = qi * jnp.exp(total - before[lo:hi])
                for h in range(heads):
                    if heads > 1:
                        m = lane_mask(span, size, h)
                        qf, qb_, qfs, qbs = (
                            jnp.where(m, x, 0.0).astype(bf16) for x in (q_f, q_b, q_fs, q_bs)
                        )
                    else:
                        qf, qb_, qfs, qbs = (x.astype(bf16) for x in (q_f, q_b, q_fs, q_bs))
                    vc = slice((head + h) * DV, (head + h + 1) * DV)
                    s_f = jnp.where(
                        row[:, :hi] + lo >= col[:, :hi], dot(qf, k_f, NT), 0.0
                    ).astype(bf16)
                    s_b = jnp.where(
                        row[:, : length - lo] <= col[:, : length - lo], dot(qb_, k_b, NT), 0.0
                    ).astype(bf16)
                    both = dot(s_f, v_ref[:hi, vc]) + dot(s_b, v_ref[lo:, vc])
                    both = both + dot(qfs, fs, NT) + dot(qbs, bs, NT)
                    scale = lax.rsqrt(jnp.mean(both * both, axis=-1, keepdims=True) + norm_eps)
                    g = g_ref[lo:hi, vc].astype(f32)
                    silu = g / (1.0 + jnp.exp(-g))
                    oc = slice(base + (head + h) * DV, base + (head + h + 1) * DV)
                    mixed[lo:hi, oc] = (both * scale * gain[...] * silu).astype(bf16)
            head += heads
        base += head * DV
    nb = wb.shape[0]
    width = out.shape[1]
    step = 512
    for c in range(0, width, step):
        out[:, c : c + step] = (
            dot(mixed[:, :nb], wb[:, c : c + step]) + dot(mixed[:, nb:], wa[:, c : c + step])
        ).astype(bf16)


def feed_kernel(n, x, *refs):
    gates, ups, downs = refs[:n], refs[n : 2 * n], refs[2 * n : 3 * n]
    out = refs[3 * n]
    rows = x.shape[1]
    step = 256
    for r in range(0, rows, step):
        g = u = None
        for i in range(n):
            xi = x[i, r : r + step, :]
            gi, ui = dot(xi, gates[i][...]), dot(xi, ups[i][...])
            g = gi if g is None else g + gi
            u = ui if u is None else u + ui
        hidden = (g / (1.0 + jnp.exp(-g)) * u).astype(bf16)
        for i in range(n):
            out[i, r : r + step, :] = dot(hidden, downs[i][...]).astype(bf16)


def call(kernel, out_shape, args, flops, scratch=()):
    size = sum(a.size * a.dtype.itemsize for a in args)
    vmem = pl.BlockSpec(memory_space=pltpu.VMEM)
    return pl.pallas_call(
        kernel,
        out_shape=out_shape,
        in_specs=[vmem] * len(args),
        out_specs=jax.tree.map(lambda _: vmem, out_shape),
        scratch_shapes=list(scratch),
        cost_estimate=pl.CostEstimate(flops=flops, bytes_accessed=size, transcendentals=0),
        compiler_params=pltpu.CompilerParams(vmem_limit_bytes=48 * 1024 * 1024),
    )(*args)


def xor_pairs(count, bit):
    return [(i, i ^ bit) for i in range(count)]


def state_scan(states, total, count, sign):
    width = states.shape[1]
    all_s, all_t = states, total
    part_s, part_t = jnp.zeros_like(states), jnp.zeros_like(total)
    hop = 1
    while hop < count:
        high = all_t.astype(bf16)
        low = (all_t - high.astype(f32)).astype(bf16)
        pad = jnp.zeros((14, width), bf16)
        packed = jnp.concatenate([all_s.astype(bf16), high, low, pad], axis=0)
        pairs = [(i, i + sign * hop) for i in range(count) if 0 <= i + sign * hop < count]
        got = lax.ppermute(packed, "sp", pairs)
        got_s = got[:DV].astype(f32)
        got_t = got[DV : DV + 1].astype(f32) + got[DV + 1 : DV + 2].astype(f32)
        part_s, part_t = part_s + got_s * jnp.exp(part_t), part_t + got_t
        all_s, all_t = all_s + got_s * jnp.exp(all_t), all_t + got_t
        hop *= 2
    return part_s


def gather_blocks(block, bits, count):
    blocks = {0: block}
    for bit in bits:
        for i in list(blocks):
            blocks[i | bit] = lax.ppermute(blocks[i], "sp", xor_pairs(count, bit))
    return blocks


def per_device(
    stream,
    first_group_queries,
    first_group_keys,
    first_group_values,
    first_gate_logits,
    first_decay_logits,
    second_group_queries,
    second_group_keys,
    second_group_values,
    second_gate_logits,
    second_decay_logits,
    position_log_decay,
    per_head_norm_gain,
    first_output_weight,
    second_output_weight,
    feedforward_norm_gain,
    gate_weight,
    up_weight,
    down_weight,
):
    n = lax.axis_size("sp")
    tp = lax.axis_size("tp")
    tokens, width = stream.shape
    me = lax.axis_index("sp")
    my_tp = lax.axis_index("tp")
    half = n // 2
    upper = me >= half

    units = gate_weight.shape[1] // 2
    low_bits = [b for b in (1 << j for j in range(20)) if b < half]

    def own_and_far(first, second, bits):
        mine = jnp.where(upper, second, first)
        theirs = jnp.where(upper, first, second)
        far = lax.ppermute(theirs, "sp", xor_pairs(n, half))
        blocks = gather_blocks(mine, bits, n)
        for i, b in gather_blocks(far, bits, n).items():
            blocks[i | half] = b
        return [blocks[i] for i in range(n)]

    gates = own_and_far(gate_weight[:, :units], gate_weight[:, units:], low_bits)
    ups = own_and_far(up_weight[:, :units], up_weight[:, units:], low_bits[::-1])
    downs = own_and_far(down_weight[:units], down_weight[units:], low_bits[::-1])

    pos = position_log_decay[:, None]
    state_width = second_group_keys.shape[1] + first_group_keys.shape[1]
    fwd, bwd, tot = call(
        states_kernel,
        (
            jax.ShapeDtypeStruct((DV, state_width), f32),
            jax.ShapeDtypeStruct((DV, state_width), f32),
            jax.ShapeDtypeStruct((8, state_width), f32),
        ),
        (
            first_group_keys,
            first_group_values,
            first_decay_logits,
            second_group_keys,
            second_group_values,
            second_decay_logits,
            pos,
        ),
        10**9,
    )
    total = tot[:1]
    fwd_in = state_scan(fwd, total, n, 1)
    bwd_in = state_scan(bwd, total, n, -1)
    heads_width = second_output_weight.shape[0] + first_output_weight.shape[0]
    partial = call(
        attend_kernel,
        jax.ShapeDtypeStruct((tokens, width), bf16),
        (
            first_group_queries,
            first_group_keys,
            first_group_values,
            first_gate_logits,
            first_decay_logits,
            second_group_queries,
            second_group_keys,
            second_group_values,
            second_gate_logits,
            second_decay_logits,
            pos,
            per_head_norm_gain[None, :],
            first_output_weight,
            second_output_weight,
            fwd_in,
            bwd_in,
        ),
        8 * 10**9,
        (pltpu.VMEM((tokens, heads_width), bf16),),
    )

    rows = tokens // tp
    arr = partial.reshape(tp, rows, width)
    bit = 1
    while bit < tp:
        arr = arr.reshape(-1, 2, rows, width)
        odd = (my_tp // bit) % 2 == 1
        keep = jnp.where(odd, arr[:, 1], arr[:, 0])
        give = jnp.where(odd, arr[:, 0], arr[:, 1]).astype(bf16)
        arr = keep.astype(f32) + lax.ppermute(give, "tp", xor_pairs(tp, bit)).astype(f32)
        bit *= 2
    own_stream = lax.dynamic_slice_in_dim(stream, my_tp * rows, rows, 0)
    residual = own_stream.astype(f32) + arr.reshape(rows, width)
    scale = lax.rsqrt(jnp.mean(residual * residual, axis=-1, keepdims=True) + norm_eps)
    normed = (residual * scale * feedforward_norm_gain).astype(bf16)

    far = lax.ppermute(normed, "sp", xor_pairs(n, half))
    arr = jnp.stack([normed, far])[None]
    bit = tp // 2
    while bit >= 1:
        got = lax.ppermute(arr, "tp", xor_pairs(tp, bit))
        arr = jnp.stack([arr, got], axis=1).reshape(-1, 2, rows, width)
        bit //= 2
    all_rows = tp * 2 * rows
    normed_all = arr.reshape(all_rows, width)
    span = width // n
    columns = jnp.stack(
        [lax.dynamic_slice_in_dim(normed_all, (me ^ i) * span, span, 1) for i in range(n)]
    )
    part = call(
        functools.partial(feed_kernel, n),
        jax.ShapeDtypeStruct((n, all_rows, span), bf16),
        (columns, *gates, *ups, *downs),
        int(6 * all_rows * width * units),
    )
    arr = part.reshape(n, tp, 2 * rows, span)
    bit = 1
    while bit < tp:
        arr = arr.reshape(n, -1, 2, 2 * rows, span)
        got = lax.ppermute(arr[:, :, 1].astype(bf16), "tp", xor_pairs(tp, bit))
        arr = arr[:, :, 0].astype(f32) + got.astype(f32)
        bit *= 2
    arr = arr.reshape(2, half, 2, rows, span)
    got = lax.ppermute(arr[:, :, 1].astype(bf16), "sp", xor_pairs(n, half))
    down = arr[:, :, 0] + got[::-1].astype(f32)
    down = down.reshape(n, rows, span)
    down_sum = jnp.concatenate(
        [lax.dynamic_index_in_dim(down, me ^ i, 0, keepdims=False) for i in range(n)], axis=1
    )
    return (residual + 0.5 * down_sum).astype(bf16)


def solution(mesh):
    in_specs = (
        P("sp", None),
        *([P("sp", "tp")] * 10),
        P("sp"),
        P(),
        P("tp", None),
        P("tp", None),
        P(),
        P("sp", "tp"),
        P("sp", "tp"),
        P("tp", "sp"),
    )
    out_specs = P(("sp", "tp"), None)
    return jax.shard_map(
        per_device, mesh=mesh, in_specs=in_specs, out_specs=out_specs, check_vma=False
    )
```

```python
import functools

import jax
import jax.numpy as jnp
from jax import lax
from jax.experimental import pallas as pl
from jax.experimental.pallas import tpu as pltpu
from jax.sharding import PartitionSpec as P

KEY_SIZE_FIRST = 64
KEY_SIZE_SECOND = 128
DV = 128
BLK = 64

decay_softness = 16.0
norm_eps = 1e-06

f32 = jnp.float32
bf16 = jnp.bfloat16
NT = (((1,), (1,)), ((), ()))
TN = (((0,), (0,)), ((), ()))


def dot(a, b, dims=None):
    if dims is None:
        return jnp.dot(a, b, preferred_element_type=f32)
    return lax.dot_general(a, b, dims, preferred_element_type=f32)


def log_decay_sums(decay_ref, pos_ref):
    x = decay_ref[...].astype(f32)
    log_decay = -jax.nn.softplus(-x) / decay_softness + pos_ref[...]
    length = x.shape[0]
    at = lax.broadcasted_iota(jnp.int32, (length, length), 0)
    of = lax.broadcasted_iota(jnp.int32, (length, length), 1)
    tri = jnp.where(at >= of, 1.0, 0.0).astype(f32)
    upto = jnp.dot(tri, log_decay, preferred_element_type=f32, precision=lax.Precision.HIGHEST)
    return upto, upto - log_decay


def lane_mask(width, key_channels, head):
    lanes = lax.broadcasted_iota(jnp.int32, (1, width), 1)
    return (lanes >= head * key_channels) & (lanes < (head + 1) * key_channels)


def head_groups(width, key_channels):
    span = min(width, 128)
    return [(s, span, span // key_channels) for s in range(0, width, span)]


def states_kernel(ka, va, da, kb, vb, db, pos, fwd, bwd, tot):
    at = 0
    for k_ref, v_ref, d_ref, size in ((kb, vb, db, KEY_SIZE_SECOND), (ka, va, da, KEY_SIZE_FIRST)):
        upto, before = log_decay_sums(d_ref, pos)
        last = upto[-1:, :]
        k = k_ref[...].astype(f32)
        ahead = (k * jnp.exp(last - upto)).astype(bf16)
        behind = (k * jnp.exp(before)).astype(bf16)
        head = 0
        for start, span, heads in head_groups(k.shape[1], size):
            f = b = None
            for h in range(heads):
                v = v_ref[:, head * DV : (head + 1) * DV]
                fh = dot(v, ahead[:, start : start + span], TN)
                bh = dot(v, behind[:, start : start + span], TN)
                if f is None:
                    f, b = fh, bh
                else:
                    m = lane_mask(span, size, h)
                    f, b = jnp.where(m, fh, f), jnp.where(m, bh, b)
                head += 1
            fwd[:, at : at + span] = f
            bwd[:, at : at + span] = b
            tot[:, at : at + span] = jnp.broadcast_to(last[:, start : start + span], (16, span))
            at += span


def attend_kernel(
    qa, ka, va, ga, da, qb, kb, vb, gb, db, pos, gain, wa, wb, fwd, bwd, out, mixed
):
    at = 0
    base = 0
    length = qa.shape[0]
    row = lax.broadcasted_iota(jnp.int32, (BLK, length), 0)
    col = lax.broadcasted_iota(jnp.int32, (BLK, length), 1)
    for q_ref, k_ref, v_ref, g_ref, d_ref, size in (
        (qb, kb, vb, gb, db, KEY_SIZE_SECOND),
        (qa, ka, va, ga, da, KEY_SIZE_FIRST),
    ):
        upto_all, before_all = log_decay_sums(d_ref, pos)
        head = 0
        for start, span, heads in head_groups(q_ref.shape[1], size):
            cut = slice(start, start + span)
            upto, before = upto_all[:, cut], before_all[:, cut]
            q = q_ref[:, cut].astype(f32)
            k = k_ref[:, cut].astype(f32)
            total = upto[-1:, :]
            fs = fwd[:, at : at + span].astype(bf16)
            bs = bwd[:, at : at + span].astype(bf16)
            at += span
            for block in range(length // BLK):
                lo, hi = block * BLK, (block + 1) * BLK
                start_log = before[lo : lo + 1, :]
                end_log = upto[hi - 1 : hi, :]
                qi = q[lo:hi]
                q_f = qi * jnp.exp(upto[lo:hi] - start_log)
                q_b = qi * jnp.exp(end_log - before[lo:hi])
                k_f = (k[:hi] * jnp.exp(start_log - upto[:hi])).astype(bf16)
                k_b = (k[lo:] * jnp.exp(before[lo:] - end_log)).astype(bf16)
                q_fs = qi * jnp.exp(upto[lo:hi])
                q_bs = qi * jnp.exp(total - before[lo:hi])
                for h in range(heads):
                    if heads > 1:
                        m = lane_mask(span, size, h)
                        qf, qb_, qfs, qbs = (
                            jnp.where(m, x, 0.0).astype(bf16) for x in (q_f, q_b, q_fs, q_bs)
                        )
                    else:
                        qf, qb_, qfs, qbs = (x.astype(bf16) for x in (q_f, q_b, q_fs, q_bs))
                    vc = slice((head + h) * DV, (head + h + 1) * DV)
                    s_f = jnp.where(
                        row[:, :hi] + lo >= col[:, :hi], dot(qf, k_f, NT), 0.0
                    ).astype(bf16)
                    s_b = jnp.where(
                        row[:, : length - lo] <= col[:, : length - lo], dot(qb_, k_b, NT), 0.0
                    ).astype(bf16)
                    both = dot(s_f, v_ref[:hi, vc]) + dot(s_b, v_ref[lo:, vc])
                    both = both + dot(qfs, fs, NT) + dot(qbs, bs, NT)
                    scale = lax.rsqrt(jnp.mean(both * both, axis=-1, keepdims=True) + norm_eps)
                    g = g_ref[lo:hi, vc].astype(f32)
                    silu = g / (1.0 + jnp.exp(-g))
                    oc = slice(base + (head + h) * DV, base + (head + h + 1) * DV)
                    mixed[lo:hi, oc] = (both * scale * gain[...] * silu).astype(bf16)
            head += heads
        base += head * DV
    nb = wb.shape[0]
    width = wb.shape[1]
    step = 512
    for c in range(0, width, step):
        part = dot(mixed[:, :nb], wb[:, c : c + step]) + dot(mixed[:, nb:], wa[:, c : c + step])
        out[:, :, :, c : c + step] = part.astype(bf16).reshape(out.shape[:3] + (step,))


def flip_bit(index, bit):
    return index + bit - 2 * bit * (index // bit % 2)


def shifted(index, mask):
    bit = 1
    while bit <= mask:
        if mask & bit:
            index = flip_bit(index, bit)
        bit *= 2
    return index


def layer_kernel(
    n,
    tp,
    stream,
    qa, ka, va, ga, da,
    qb, kb, vb, gb, db,
    pos,
    gain,
    wa, wb,
    norm_gain,
    mine_g, mine_u, mine_d,
    far_g, far_u, far_d,
    out,
    weights_g, weights_u, weights_d,
    grp_f, grp_b, pre_f, pre_b, tot,
    scan_out, scan_in,
    mixed, partial, residual, rows_all, gate_acc, down_part,
    *rest,
):
    levels = tp.bit_length() - 1
    rest = list(rest)
    recv1 = [rest.pop(0) for _ in range(levels)]
    send1 = [rest.pop(0) for _ in range(levels - 1)]
    recv2 = [rest.pop(0) for _ in range(levels)]
    send2 = [rest.pop(0) for _ in range(levels - 1)]
    acc = [rest.pop(0) for _ in range(levels - 1)]
    last_out, last_in, hidden, w_sem, scan_sem, tp_sem, row_sem, last_sem, own_sem = rest
    me = lax.axis_index("sp")
    my_tp = lax.axis_index("tp")
    half = n // 2
    sp_bits = [1 << j for j in range(n.bit_length() - 1)]
    tp_bits = [1 << j for j in range(levels)]
    rows = residual.shape[0]

    barrier = pltpu.get_barrier_semaphore()
    for bit in sp_bits:
        pl.semaphore_signal(
            barrier, inc=1, device_id={"sp": flip_bit(me, bit)}, device_id_type=pl.DeviceIdType.MESH
        )
    for bit in tp_bits:
        pl.semaphore_signal(
            barrier,
            inc=1,
            device_id={"tp": flip_bit(my_tp, bit)},
            device_id_type=pl.DeviceIdType.MESH,
        )
    pl.semaphore_wait(barrier, len(sp_bits) + len(tp_bits))

    def remote(src, dst, sems, axis, bit):
        place = me if axis == "sp" else my_tp
        return pltpu.make_async_remote_copy(
            src_ref=src,
            dst_ref=dst,
            send_sem=sems[0],
            recv_sem=sems[1],
            device_id={axis: flip_bit(place, bit)},
            device_id_type=pl.DeviceIdType.MESH,
        )

    low = [b for b in sp_bits if b < half]
    weights = (
        (weights_g, mine_g, far_g, low),
        (weights_u, mine_u, far_u, low[::-1]),
        (weights_d, mine_d, far_d, low[::-1]),
    )
    copies = {}

    def send(w, at, bit):
        store, mine, far, _ = weights[w]
        if bit == half:
            src = far
        elif at == 0:
            src = mine
        else:
            src = store.at[shifted(me, at)]
        place = me if at == 0 else shifted(me, at)
        sems = (w_sem.at[0, w, at | bit], w_sem.at[1, w, at | bit])
        copies[w, at | bit] = remote(src, store.at[place], sems, "sp", bit)
        copies[w, at | bit].start()

    sent = set()

    def offer(w, at, bit):
        if (w, at, bit) not in sent:
            sent.add((w, at, bit))
            send(w, at, bit)

    def onward(w, at):
        order = weights[w][3]
        low_part = at & (half - 1)
        used = [order.index(b) for b in order if low_part & b]
        return order[max(used) + 1 if used else 0 :]

    own = [
        pltpu.make_async_copy(mine, store.at[me], own_sem.at[i])
        for i, (store, mine, _, _) in enumerate(weights)
    ]
    for copy in own:
        copy.start()
    for w in (0, 1):
        offer(w, 0, half)
        offer(w, 0, low[0])

    states_kernel(ka, va, da, kb, vb, db, pos, grp_f, grp_b, tot)
    pre_f[...] = jnp.zeros_like(pre_f)
    pre_b[...] = jnp.zeros_like(pre_b)
    before = jnp.zeros((1, tot.shape[1]), f32)
    after = before
    group = tot[0:1]
    for step, bit in enumerate(sp_bits):
        high = group.astype(bf16)
        rest_of = (group - high.astype(f32)).astype(bf16)
        scan_out[step, :DV] = grp_f[...].astype(bf16)
        scan_out[step, DV : 2 * DV] = grp_b[...].astype(bf16)
        scan_out[step, 2 * DV : 2 * DV + 16] = jnp.broadcast_to(high.astype(f32), tot.shape).astype(bf16)
        scan_out[step, 2 * DV + 16 :] = jnp.broadcast_to(rest_of.astype(f32), tot.shape).astype(bf16)
        copy = remote(
            scan_out.at[step],
            scan_in.at[step],
            (scan_sem.at[0, step], scan_sem.at[1, step]),
            "sp",
            bit,
        )
        copy.start()
        copy.wait()
        got_f = scan_in[step, :DV].astype(f32)
        got_b = scan_in[step, DV : 2 * DV].astype(f32)
        got_t = (
            scan_in[step, 2 * DV : 2 * DV + 16].astype(f32)
            + scan_in[step, 2 * DV + 16 :].astype(f32)
        )[0:1]
        up = jnp.full((1, tot.shape[1]), me // bit % 2, jnp.int32).astype(f32)
        down = 1.0 - up
        pre_f[...] += got_f * (up * jnp.exp(before))
        pre_b[...] += got_b * (down * jnp.exp(after))
        before, after = before + up * got_t, after + down * got_t
        grp_f[...] = grp_f[...] * jnp.exp(down * got_t) + got_f * jnp.exp(up * group)
        grp_b[...] = grp_b[...] * jnp.exp(up * got_t) + got_b * jnp.exp(down * group)
        group = group + got_t
        if step == 0:
            offer(0, 0, low[-1])
        if step == 1:
            offer(2, 0, half)
    for w in range(3):
        offer(w, 0, half)
        for bit in low:
            offer(w, 0, bit) if bit in onward(w, 0) else None

    attend_kernel(
        qa, ka, va, ga, da, qb, kb, vb, gb, db, pos, gain, wa, wb, pre_f, pre_b, partial, mixed
    )

    arrived = set()

    def take(w, at):
        if at == 0 or (w, at) in arrived:
            return
        arrived.add((w, at))
        copies[w, at].wait_recv()
        for bit in onward(w, at):
            offer(w, at, bit)

    def tp_sum(part, recvs, sends, number):
        value = None
        for j, bit in enumerate(tp_bits):
            odd = my_tp // bit % 2
            src = part if j == 0 else sends[j - 1]
            copy = remote(
                src.at[:, 1 - odd],
                recvs[j],
                (tp_sem.at[0, number, j], tp_sem.at[1, number, j]),
                "tp",
                bit,
            )
            copy.start()
            yield
            copy.wait()
            size = recvs[j].shape[1]
            if j == 0:
                kept = part[:, pl.ds(odd, 1)]
            else:
                kept = acc[j - 1][:, pl.ds(odd, 1), :size]
            value = kept[:, 0].astype(f32) + recvs[j][...].astype(f32)
            if j < levels - 1:
                shape = (value.shape[0] // 2, 2) + value.shape[1:]
                acc[j][:, :, :size] = value.reshape(shape)
                sends[j][...] = value.astype(bf16).reshape(shape)
        yield value[0]

    def run(gen, between):
        value = None
        for j, value in enumerate(gen):
            if value is None and j < len(between):
                for w, at in between[j]:
                    take(w, at)
        return value

    summed = run(tp_sum(partial, recv1, send1, 0), [[(0, half), (1, half)], [(0, low[0])]])
    own_rows = pl.ds(pl.multiple_of(my_tp * rows, rows), rows)
    res = stream[own_rows, :].astype(f32) + summed
    residual[...] = res
    scale = lax.rsqrt(jnp.mean(res * res, axis=-1, keepdims=True) + norm_eps)
    rows_all[0, my_tp] = (res * scale * norm_gain[...]).astype(bf16)

    row_copies = {}

    def pass_rows(part, at, bit):
        place = shifted(my_tp, at) if at else my_tp
        ref = rows_all.at[part, place]
        number = part * tp + (at | bit)
        row_copies[part, at | bit] = remote(
            ref, ref, (row_sem.at[0, number], row_sem.at[1, number]), "tp", bit
        )
        row_copies[part, at | bit].start()

    across = remote(
        rows_all.at[0, my_tp],
        rows_all.at[1, my_tp],
        (row_sem.at[0, tp * 2], row_sem.at[1, tp * 2]),
        "sp",
        half,
    )
    across.start()
    for bit in tp_bits[::-1]:
        pass_rows(0, 0, bit)
    for w, at in ((0, low[0]), (1, half), (1, low[0]), (2, half)):
        take(w, at)
    across.wait_recv()
    for bit in tp_bits[::-1]:
        pass_rows(1, 0, bit)
    for bit in tp_bits[-2::-1]:
        for part in (0, 1):
            for at in [a for a in range(1, tp) if a % (2 * bit) == 0]:
                if not row_copies.get(("got", part, at)):
                    row_copies["got", part, at] = True
                    row_copies[part, at].wait_recv()
                pass_rows(part, at, bit)

    def by_arrival(w):
        order = weights[w][3]
        return sorted(range(1, n), key=lambda i: ((i & (half - 1)).bit_count(), i < half, i))

    first = [i for i in by_arrival(0) if (i & (half - 1)).bit_count() <= 1]
    for i in first:
        for w in range(3):
            take(w, i)
    for part in (0, 1):
        for at in range(1, tp):
            if not row_copies.get(("got", part, at)):
                row_copies["got", part, at] = True
                row_copies[part, at].wait_recv()
    for copy in own:
        copy.wait()

    span = weights_g.shape[1]
    flat = tp * rows

    def project(w, store, part):
        x = rows_all[part].reshape(flat, n * span)
        total = None
        for j in range(n):
            term = dot(x[:, j * span : (j + 1) * span], store[j])
            total = term if total is None else total + term
        return total

    for i in by_arrival(0):
        take(0, i)
    for part in (0, 1):
        gate_acc[part] = project(0, weights_g, part)
    for i in by_arrival(1):
        take(1, i)
    for part in (0, 1):
        g = gate_acc[part]
        u = project(1, weights_u, part)
        hidden[part] = (g / (1.0 + jnp.exp(-g)) * u).astype(bf16)
    for i in by_arrival(2):
        take(2, i)
    for part in (0, 1):
        for j in range(n):
            value = dot(hidden[part], weights_d[j]).astype(bf16)
            down_part[:, :, part * rows : (part + 1) * rows, j * span : (j + 1) * span] = (
                value.reshape(tp // 2, 2, rows, span)
            )
    value = run(tp_sum(down_part, recv2, send2, 1), [])
    last_out[...] = value[rows:].astype(bf16)
    residual[...] += 0.5 * value[:rows]
    copy = remote(last_out, last_in, (last_sem.at[0], last_sem.at[1]), "sp", half)
    copy.start()
    copy.wait()
    out[...] = (residual[...] + 0.5 * last_in[...].astype(f32)).astype(bf16)
    for copy in copies.values():
        copy.wait_send()
    for key, copy in row_copies.items():
        if key[0] != "got":
            copy.wait_send()
    across.wait_send()


def per_device(
    stream,
    first_group_queries,
    first_group_keys,
    first_group_values,
    first_gate_logits,
    first_decay_logits,
    second_group_queries,
    second_group_keys,
    second_group_values,
    second_gate_logits,
    second_decay_logits,
    position_log_decay,
    per_head_norm_gain,
    first_output_weight,
    second_output_weight,
    feedforward_norm_gain,
    gate_weight,
    up_weight,
    down_weight,
):
    n = lax.axis_size("sp")
    tp = lax.axis_size("tp")
    tokens, width = stream.shape
    upper = lax.axis_index("sp") >= n // 2
    units = gate_weight.shape[1] // 2
    rows = tokens // tp
    span = width // n

    def halves(first, second):
        return jnp.where(upper, second, first), jnp.where(upper, first, second)

    mine_g, far_g = halves(gate_weight[:, :units], gate_weight[:, units:])
    mine_u, far_u = halves(up_weight[:, :units], up_weight[:, units:])
    mine_d, far_d = halves(down_weight[:units], down_weight[units:])
    args = (
        stream,
        first_group_queries,
        first_group_keys,
        first_group_values,
        first_gate_logits,
        first_decay_logits,
        second_group_queries,
        second_group_keys,
        second_group_values,
        second_gate_logits,
        second_decay_logits,
        position_log_decay[:, None],
        per_head_norm_gain[None, :],
        first_output_weight,
        second_output_weight,
        feedforward_norm_gain[None, :],
        mine_g,
        mine_u,
        mine_d,
        far_g,
        far_u,
        far_d,
    )
    states = second_group_keys.shape[1] + first_group_keys.shape[1]
    heads_width = second_output_weight.shape[0] + first_output_weight.shape[0]
    levels = tp.bit_length() - 1
    steps = n.bit_length() - 1
    vm = pltpu.VMEM

    def tp_buffers(size):
        recv = [vm((tp >> (j + 1), size, width), bf16) for j in range(levels)]
        give = [vm((tp >> (j + 2), 2, size, width), bf16) for j in range(levels - 1)]
        return recv + give

    scratch = [
        vm((n, span, units), bf16),
        vm((n, span, units), bf16),
        vm((n, units, span), bf16),
        *([vm((DV, states), f32)] * 4),
        vm((16, states), f32),
        vm((steps, 2 * DV + 32, states), bf16),
        vm((steps, 2 * DV + 32, states), bf16),
        vm((tokens, heads_width), bf16),
        vm((tp // 2, 2, rows, width), bf16),
        vm((rows, width), f32),
        vm((2, tp, rows, width), bf16),
        vm((2, tokens, units), f32),
        vm((tp // 2, 2, 2 * rows, width), bf16),
        *tp_buffers(rows),
        *tp_buffers(2 * rows),
        *[vm((tp >> (j + 2), 2, 2 * rows, width), f32) for j in range(levels - 1)],
        vm((rows, width), bf16),
        vm((rows, width), bf16),
        vm((2, tokens, units), bf16),
        pltpu.SemaphoreType.DMA((2, 3, n)),
        pltpu.SemaphoreType.DMA((2, steps)),
        pltpu.SemaphoreType.DMA((2, 2, levels)),
        pltpu.SemaphoreType.DMA((2, 2 * tp + 1)),
        pltpu.SemaphoreType.DMA((2,)),
        pltpu.SemaphoreType.DMA((3,)),
    ]
    spec = pl.BlockSpec(memory_space=pltpu.VMEM)
    return pl.pallas_call(
        functools.partial(layer_kernel, n, tp),
        out_shape=jax.ShapeDtypeStruct((rows, width), bf16),
        in_specs=[spec] * len(args),
        out_specs=spec,
        scratch_shapes=scratch,
        compiler_params=pltpu.CompilerParams(
            collective_id=0, has_side_effects=True, vmem_limit_bytes=60 * 1024 * 1024
        ),
    )(*args)


def solution(mesh):
    in_specs = (
        P("sp", None),
        *([P("sp", "tp")] * 10),
        P("sp"),
        P(),
        P("tp", None),
        P("tp", None),
        P(),
        P("sp", "tp"),
        P("sp", "tp"),
        P("tp", "sp"),
    )
    out_specs = P(("sp", "tp"), None)
    return jax.shard_map(
        per_device, mesh=mesh, in_specs=in_specs, out_specs=out_specs, check_vma=False
    )
```

```python
import functools

import jax
import jax.numpy as jnp
from jax import lax
from jax.experimental import pallas as pl
from jax.experimental.pallas import tpu as pltpu
from jax.sharding import PartitionSpec as P

KEY_SIZE_FIRST = 64
KEY_SIZE_SECOND = 128
DV = 128
BLK = 64

decay_softness = 16.0
norm_eps = 1e-06

f32 = jnp.float32
bf16 = jnp.bfloat16
NT = (((1,), (1,)), ((), ()))
TN = (((0,), (0,)), ((), ()))


def dot(a, b, dims=None):
    if dims is None:
        return jnp.dot(a, b, preferred_element_type=f32)
    return lax.dot_general(a, b, dims, preferred_element_type=f32)


def log_decay_sums(decay_ref, pos_ref):
    x = decay_ref[...].astype(f32)
    log_decay = -jax.nn.softplus(-x) / decay_softness + pos_ref[...]
    length = x.shape[0]
    at = lax.broadcasted_iota(jnp.int32, (length, length), 0)
    of = lax.broadcasted_iota(jnp.int32, (length, length), 1)
    tri = jnp.where(at >= of, 1.0, 0.0).astype(f32)
    upto = jnp.dot(tri, log_decay, preferred_element_type=f32, precision=lax.Precision.HIGHEST)
    return upto, upto - log_decay


def lane_mask(width, key_channels, head):
    lanes = lax.broadcasted_iota(jnp.int32, (1, width), 1)
    return (lanes >= head * key_channels) & (lanes < (head + 1) * key_channels)


def head_groups(width, key_channels):
    span = min(width, 128)
    return [(s, span, span // key_channels) for s in range(0, width, span)]


def states_kernel(ka, va, da, kb, vb, db, pos, fwd, bwd, tot):
    at = 0
    for k_ref, v_ref, d_ref, size in ((kb, vb, db, KEY_SIZE_SECOND), (ka, va, da, KEY_SIZE_FIRST)):
        upto, before = log_decay_sums(d_ref, pos)
        last = upto[-1:, :]
        k = k_ref[...].astype(f32)
        ahead = (k * jnp.exp(last - upto)).astype(bf16)
        behind = (k * jnp.exp(before)).astype(bf16)
        head = 0
        for start, span, heads in head_groups(k.shape[1], size):
            f = b = None
            for h in range(heads):
                v = v_ref[:, head * DV : (head + 1) * DV]
                fh = dot(v, ahead[:, start : start + span], TN)
                bh = dot(v, behind[:, start : start + span], TN)
                if f is None:
                    f, b = fh, bh
                else:
                    m = lane_mask(span, size, h)
                    f, b = jnp.where(m, fh, f), jnp.where(m, bh, b)
                head += 1
            fwd[:, at : at + span] = f
            bwd[:, at : at + span] = b
            tot[:, at : at + span] = jnp.broadcast_to(last[:, start : start + span], (16, span))
            at += span


def attend_kernel(
    qa, ka, va, ga, da, qb, kb, vb, gb, db, pos, gain, wa, wb, fwd, bwd, out, mixed
):
    at = 0
    base = 0
    length = qa.shape[0]
    row = lax.broadcasted_iota(jnp.int32, (BLK, length), 0)
    col = lax.broadcasted_iota(jnp.int32, (BLK, length), 1)
    for q_ref, k_ref, v_ref, g_ref, d_ref, size in (
        (qb, kb, vb, gb, db, KEY_SIZE_SECOND),
        (qa, ka, va, ga, da, KEY_SIZE_FIRST),
    ):
        upto_all, before_all = log_decay_sums(d_ref, pos)
        head = 0
        for start, span, heads in head_groups(q_ref.shape[1], size):
            cut = slice(start, start + span)
            upto, before = upto_all[:, cut], before_all[:, cut]
            q = q_ref[:, cut].astype(f32)
            k = k_ref[:, cut].astype(f32)
            total = upto[-1:, :]
            fs = fwd[:, at : at + span].astype(bf16)
            bs = bwd[:, at : at + span].astype(bf16)
            at += span
            for block in range(length // BLK):
                lo, hi = block * BLK, (block + 1) * BLK
                start_log = before[lo : lo + 1, :]
                end_log = upto[hi - 1 : hi, :]
                qi = q[lo:hi]
                q_f = qi * jnp.exp(upto[lo:hi] - start_log)
                q_b = qi * jnp.exp(end_log - before[lo:hi])
                k_f = (k[:hi] * jnp.exp(start_log - upto[:hi])).astype(bf16)
                k_b = (k[lo:] * jnp.exp(before[lo:] - end_log)).astype(bf16)
                q_fs = qi * jnp.exp(upto[lo:hi])
                q_bs = qi * jnp.exp(total - before[lo:hi])
                for h in range(heads):
                    if heads > 1:
                        m = lane_mask(span, size, h)
                        qf, qb_, qfs, qbs = (
                            jnp.where(m, x, 0.0).astype(bf16) for x in (q_f, q_b, q_fs, q_bs)
                        )
                    else:
                        qf, qb_, qfs, qbs = (x.astype(bf16) for x in (q_f, q_b, q_fs, q_bs))
                    vc = slice((head + h) * DV, (head + h + 1) * DV)
                    s_f = jnp.where(
                        row[:, :hi] + lo >= col[:, :hi], dot(qf, k_f, NT), 0.0
                    ).astype(bf16)
                    s_b = jnp.where(
                        row[:, : length - lo] <= col[:, : length - lo], dot(qb_, k_b, NT), 0.0
                    ).astype(bf16)
                    both = dot(s_f, v_ref[:hi, vc]) + dot(s_b, v_ref[lo:, vc])
                    both = both + dot(qfs, fs, NT) + dot(qbs, bs, NT)
                    scale = lax.rsqrt(jnp.mean(both * both, axis=-1, keepdims=True) + norm_eps)
                    g = g_ref[lo:hi, vc].astype(f32)
                    silu = g / (1.0 + jnp.exp(-g))
                    oc = slice(base + (head + h) * DV, base + (head + h + 1) * DV)
                    mixed[lo:hi, oc] = (both * scale * gain[...] * silu).astype(bf16)
            head += heads
        base += head * DV
    nb = wb.shape[0]
    width = wb.shape[1]
    step = 512
    for c in range(0, width, step):
        part = dot(mixed[:, :nb], wb[:, c : c + step]) + dot(mixed[:, nb:], wa[:, c : c + step])
        out[:, :, :, c : c + step] = part.astype(bf16).reshape(out.shape[:3] + (step,))


def flip_bit(index, bit):
    return index + bit - 2 * bit * (index // bit % 2)


def shifted(index, mask):
    bit = 1
    while bit <= mask:
        if mask & bit:
            index = flip_bit(index, bit)
        bit *= 2
    return index


def layer_kernel(
    n,
    tp,
    stream,
    qa, ka, va, ga, da,
    qb, kb, vb, gb, db,
    pos,
    gain,
    wa, wb,
    norm_gain,
    mine_g, mine_u, mine_d,
    far_g, far_u, far_d,
    out,
    weights_g, weights_u, weights_d,
    grp_f, grp_b, pre_f, pre_b, tot,
    scan_out, scan_in,
    mixed, partial, residual, rows_all, gate_acc, down_part,
    *rest,
):
    levels = tp.bit_length() - 1
    rest = list(rest)
    recv1 = [rest.pop(0) for _ in range(levels)]
    send1 = [rest.pop(0) for _ in range(levels - 1)]
    recv2 = [rest.pop(0) for _ in range(levels)]
    send2 = [rest.pop(0) for _ in range(levels - 1)]
    acc = [rest.pop(0) for _ in range(levels - 1)]
    last_out, last_in, hidden, w_sem, scan_sem, tp_sem, row_sem, last_sem, own_sem = rest
    me = lax.axis_index("sp")
    my_tp = lax.axis_index("tp")
    half = n // 2
    sp_bits = [1 << j for j in range(n.bit_length() - 1)]
    tp_bits = [1 << j for j in range(levels)]
    rows = residual.shape[0]

    barrier = pltpu.get_barrier_semaphore()
    for bit in sp_bits:
        pl.semaphore_signal(
            barrier, inc=1, device_id={"sp": flip_bit(me, bit)}, device_id_type=pl.DeviceIdType.MESH
        )
    for bit in tp_bits:
        pl.semaphore_signal(
            barrier,
            inc=1,
            device_id={"tp": flip_bit(my_tp, bit)},
            device_id_type=pl.DeviceIdType.MESH,
        )
    pl.semaphore_wait(barrier, len(sp_bits) + len(tp_bits))

    def remote(src, dst, sems, axis, bit):
        place = me if axis == "sp" else my_tp
        return pltpu.make_async_remote_copy(
            src_ref=src,
            dst_ref=dst,
            send_sem=sems[0],
            recv_sem=sems[1],
            device_id={axis: flip_bit(place, bit)},
            device_id_type=pl.DeviceIdType.MESH,
        )

    low = [b for b in sp_bits if b < half]
    weights = (
        (weights_g, mine_g, far_g, low),
        (weights_u, mine_u, far_u, low[::-1]),
        (weights_d, mine_d, far_d, low[::-1]),
    )
    copies = {}

    def send(w, at, bit):
        store, mine, far, _ = weights[w]
        if bit == half:
            src = far
        elif at == 0:
            src = mine
        else:
            src = store.at[shifted(me, at)]
        place = me if at == 0 else shifted(me, at)
        sems = (w_sem.at[0, w, at | bit], w_sem.at[1, w, at | bit])
        copies[w, at | bit] = remote(src, store.at[place], sems, "sp", bit)
        copies[w, at | bit].start()

    sent = set()

    def offer(w, at, bit):
        if (w, at, bit) not in sent:
            sent.add((w, at, bit))
            send(w, at, bit)

    def onward(w, at):
        order = weights[w][3]
        low_part = at & (half - 1)
        used = [order.index(b) for b in order if low_part & b]
        return order[max(used) + 1 if used else 0 :]

    own = [
        pltpu.make_async_copy(mine, store.at[me], own_sem.at[i])
        for i, (store, mine, _, _) in enumerate(weights)
    ]
    for copy in own:
        copy.start()
    for w in (0, 1, 2):
        offer(w, 0, half)
        for bit in low:
            offer(w, 0, bit)

    states_kernel(ka, va, da, kb, vb, db, pos, grp_f, grp_b, tot)
    pre_f[...] = jnp.zeros_like(pre_f)
    pre_b[...] = jnp.zeros_like(pre_b)
    before = jnp.zeros((1, tot.shape[1]), f32)
    after = before
    group = tot[0:1]
    for step, bit in enumerate(sp_bits):
        high = group.astype(bf16)
        rest_of = (group - high.astype(f32)).astype(bf16)
        scan_out[step, :DV] = grp_f[...].astype(bf16)
        scan_out[step, DV : 2 * DV] = grp_b[...].astype(bf16)
        scan_out[step, 2 * DV : 2 * DV + 16] = jnp.broadcast_to(high.astype(f32), tot.shape).astype(bf16)
        scan_out[step, 2 * DV + 16 :] = jnp.broadcast_to(rest_of.astype(f32), tot.shape).astype(bf16)
        copy = remote(
            scan_out.at[step],
            scan_in.at[step],
            (scan_sem.at[0, step], scan_sem.at[1, step]),
            "sp",
            bit,
        )
        copy.start()
        copy.wait()
        got_f = scan_in[step, :DV].astype(f32)
        got_b = scan_in[step, DV : 2 * DV].astype(f32)
        got_t = (
            scan_in[step, 2 * DV : 2 * DV + 16].astype(f32)
            + scan_in[step, 2 * DV + 16 :].astype(f32)
        )[0:1]
        up = jnp.full((1, tot.shape[1]), me // bit % 2, jnp.int32).astype(f32)
        down = 1.0 - up
        pre_f[...] += got_f * (up * jnp.exp(before))
        pre_b[...] += got_b * (down * jnp.exp(after))
        before, after = before + up * got_t, after + down * got_t
        grp_f[...] = grp_f[...] * jnp.exp(down * got_t) + got_f * jnp.exp(up * group)
        grp_b[...] = grp_b[...] * jnp.exp(up * got_t) + got_b * jnp.exp(down * group)
        group = group + got_t
        if step == 0:
            offer(0, 0, low[-1])
        if step == 1:
            offer(2, 0, half)
    for w in range(3):
        offer(w, 0, half)
        for bit in low:
            offer(w, 0, bit) if bit in onward(w, 0) else None

    attend_kernel(
        qa, ka, va, ga, da, qb, kb, vb, gb, db, pos, gain, wa, wb, pre_f, pre_b, partial, mixed
    )

    arrived = set()

    def take(w, at):
        if at == 0 or (w, at) in arrived:
            return
        arrived.add((w, at))
        copies[w, at].wait_recv()
        for bit in onward(w, at):
            offer(w, at, bit)

    def tp_sum(part, recvs, sends, number):
        value = None
        for j, bit in enumerate(tp_bits):
            odd = my_tp // bit % 2
            src = part if j == 0 else sends[j - 1]
            copy = remote(
                src.at[:, 1 - odd],
                recvs[j],
                (tp_sem.at[0, number, j], tp_sem.at[1, number, j]),
                "tp",
                bit,
            )
            copy.start()
            yield
            copy.wait()
            size = recvs[j].shape[1]
            if j == 0:
                kept = part[:, pl.ds(odd, 1)]
            else:
                kept = acc[j - 1][:, pl.ds(odd, 1), :size]
            value = kept[:, 0].astype(f32) + recvs[j][...].astype(f32)
            if j < levels - 1:
                shape = (value.shape[0] // 2, 2) + value.shape[1:]
                acc[j][:, :, :size] = value.reshape(shape)
                sends[j][...] = value.astype(bf16).reshape(shape)
        yield value[0]

    def run(gen, between):
        value = None
        for j, value in enumerate(gen):
            if value is None and j < len(between):
                for w, at in between[j]:
                    take(w, at)
        return value

    summed = run(tp_sum(partial, recv1, send1, 0), [[(0, half), (1, half)], [(0, low[0])]])
    own_rows = pl.ds(pl.multiple_of(my_tp * rows, rows), rows)
    res = stream[own_rows, :].astype(f32) + summed
    residual[...] = res
    scale = lax.rsqrt(jnp.mean(res * res, axis=-1, keepdims=True) + norm_eps)
    rows_all[0, my_tp] = (res * scale * norm_gain[...]).astype(bf16)

    row_copies = {}

    def pass_rows(part, at, bit):
        place = shifted(my_tp, at) if at else my_tp
        ref = rows_all.at[part, place]
        number = part * tp + (at | bit)
        row_copies[part, at | bit] = remote(
            ref, ref, (row_sem.at[0, number], row_sem.at[1, number]), "tp", bit
        )
        row_copies[part, at | bit].start()

    across = remote(
        rows_all.at[0, my_tp],
        rows_all.at[1, my_tp],
        (row_sem.at[0, tp * 2], row_sem.at[1, tp * 2]),
        "sp",
        half,
    )
    across.start()
    for bit in tp_bits[::-1]:
        pass_rows(0, 0, bit)
    for w, at in ((0, low[0]), (1, half), (1, low[0]), (2, half)):
        take(w, at)
    across.wait_recv()
    for bit in tp_bits[::-1]:
        pass_rows(1, 0, bit)
    for bit in tp_bits[-2::-1]:
        for part in (0, 1):
            for at in [a for a in range(1, tp) if a % (2 * bit) == 0]:
                if not row_copies.get(("got", part, at)):
                    row_copies["got", part, at] = True
                    row_copies[part, at].wait_recv()
                pass_rows(part, at, bit)

    def by_arrival(w):
        order = weights[w][3]
        return sorted(range(1, n), key=lambda i: ((i & (half - 1)).bit_count(), i < half, i))

    first = [i for i in by_arrival(0) if (i & (half - 1)).bit_count() <= 1]
    for i in first:
        for w in range(3):
            take(w, i)
    for part in (0, 1):
        for at in range(1, tp):
            if not row_copies.get(("got", part, at)):
                row_copies["got", part, at] = True
                row_copies[part, at].wait_recv()
    for copy in own:
        copy.wait()

    span = weights_g.shape[1]
    flat = tp * rows

    def project(w, store, part):
        x = rows_all[part].reshape(flat, n * span)
        total = None
        for j in range(n):
            term = dot(x[:, j * span : (j + 1) * span], store[j])
            total = term if total is None else total + term
        return total

    for i in by_arrival(0):
        take(0, i)
    for part in (0, 1):
        gate_acc[part] = project(0, weights_g, part)
    for i in by_arrival(1):
        take(1, i)
    for part in (0, 1):
        g = gate_acc[part]
        u = project(1, weights_u, part)
        hidden[part] = (g / (1.0 + jnp.exp(-g)) * u).astype(bf16)
    for i in by_arrival(2):
        take(2, i)
    for part in (0, 1):
        for j in range(n):
            value = dot(hidden[part], weights_d[j]).astype(bf16)
            down_part[:, :, part * rows : (part + 1) * rows, j * span : (j + 1) * span] = (
                value.reshape(tp // 2, 2, rows, span)
            )
    value = run(tp_sum(down_part, recv2, send2, 1), [])
    last_out[...] = value[rows:].astype(bf16)
    residual[...] += 0.5 * value[:rows]
    copy = remote(last_out, last_in, (last_sem.at[0], last_sem.at[1]), "sp", half)
    copy.start()
    copy.wait()
    out[...] = (residual[...] + 0.5 * last_in[...].astype(f32)).astype(bf16)
    for copy in copies.values():
        copy.wait_send()
    for key, copy in row_copies.items():
        if key[0] != "got":
            copy.wait_send()
    across.wait_send()


def per_device(
    stream,
    first_group_queries,
    first_group_keys,
    first_group_values,
    first_gate_logits,
    first_decay_logits,
    second_group_queries,
    second_group_keys,
    second_group_values,
    second_gate_logits,
    second_decay_logits,
    position_log_decay,
    per_head_norm_gain,
    first_output_weight,
    second_output_weight,
    feedforward_norm_gain,
    gate_weight,
    up_weight,
    down_weight,
):
    n = lax.axis_size("sp")
    tp = lax.axis_size("tp")
    tokens, width = stream.shape
    upper = lax.axis_index("sp") >= n // 2
    units = gate_weight.shape[1] // 2
    rows = tokens // tp
    span = width // n

    def halves(first, second):
        return jnp.where(upper, second, first), jnp.where(upper, first, second)

    mine_g, far_g = halves(gate_weight[:, :units], gate_weight[:, units:])
    mine_u, far_u = halves(up_weight[:, :units], up_weight[:, units:])
    mine_d, far_d = halves(down_weight[:units], down_weight[units:])
    args = (
        stream,
        first_group_queries,
        first_group_keys,
        first_group_values,
        first_gate_logits,
        first_decay_logits,
        second_group_queries,
        second_group_keys,
        second_group_values,
        second_gate_logits,
        second_decay_logits,
        position_log_decay[:, None],
        per_head_norm_gain[None, :],
        first_output_weight,
        second_output_weight,
        feedforward_norm_gain[None, :],
        mine_g,
        mine_u,
        mine_d,
        far_g,
        far_u,
        far_d,
    )
    states = second_group_keys.shape[1] + first_group_keys.shape[1]
    heads_width = second_output_weight.shape[0] + first_output_weight.shape[0]
    levels = tp.bit_length() - 1
    steps = n.bit_length() - 1
    vm = pltpu.VMEM

    def tp_buffers(size):
        recv = [vm((tp >> (j + 1), size, width), bf16) for j in range(levels)]
        give = [vm((tp >> (j + 2), 2, size, width), bf16) for j in range(levels - 1)]
        return recv + give

    scratch = [
        vm((n, span, units), bf16),
        vm((n, span, units), bf16),
        vm((n, units, span), bf16),
        *([vm((DV, states), f32)] * 4),
        vm((16, states), f32),
        vm((steps, 2 * DV + 32, states), bf16),
        vm((steps, 2 * DV + 32, states), bf16),
        vm((tokens, heads_width), bf16),
        vm((tp // 2, 2, rows, width), bf16),
        vm((rows, width), f32),
        vm((2, tp, rows, width), bf16),
        vm((2, tokens, units), f32),
        vm((tp // 2, 2, 2 * rows, width), bf16),
        *tp_buffers(rows),
        *tp_buffers(2 * rows),
        *[vm((tp >> (j + 2), 2, 2 * rows, width), f32) for j in range(levels - 1)],
        vm((rows, width), bf16),
        vm((rows, width), bf16),
        vm((2, tokens, units), bf16),
        pltpu.SemaphoreType.DMA((2, 3, n)),
        pltpu.SemaphoreType.DMA((2, steps)),
        pltpu.SemaphoreType.DMA((2, 2, levels)),
        pltpu.SemaphoreType.DMA((2, 2 * tp + 1)),
        pltpu.SemaphoreType.DMA((2,)),
        pltpu.SemaphoreType.DMA((3,)),
    ]
    spec = pl.BlockSpec(memory_space=pltpu.VMEM)
    return pl.pallas_call(
        functools.partial(layer_kernel, n, tp),
        out_shape=jax.ShapeDtypeStruct((rows, width), bf16),
        in_specs=[spec] * len(args),
        out_specs=spec,
        scratch_shapes=scratch,
        compiler_params=pltpu.CompilerParams(
            collective_id=0, has_side_effects=True, vmem_limit_bytes=60 * 1024 * 1024
        ),
    )(*args)


def solution(mesh):
    in_specs = (
        P("sp", None),
        *([P("sp", "tp")] * 10),
        P("sp"),
        P(),
        P("tp", None),
        P("tp", None),
        P(),
        P("sp", "tp"),
        P("sp", "tp"),
        P("tp", "sp"),
    )
    out_specs = P(("sp", "tp"), None)
    return jax.shard_map(
        per_device, mesh=mesh, in_specs=in_specs, out_specs=out_specs, check_vma=False
    )
```
